512 devices in a mesh: sp: 64 (over z, y), tp: 8 (over x, core).
Axes of the slice: x: 4, y: 8, z: 8, core: 2. Of those that a mesh axis runs over, the one named last changes fastest.
Arguments:
- hidden_in: bfloat16 [24576, 2048], P('sp'), may hold values from -6 to 6
- drive: bfloat16 [24576, 1024], P('sp', 'tp'), may hold values from -24 to 24
- wide_poles: float32 [2, 32, 64], P(None, 'tp'), may hold values from -2 to 256, as said below
- narrow_poles: float32 [2, 32, 32], P(None, 'tp'), may hold values from -2 to 128, as said below
- log_step: float32 [32, 2], P('tp'), may hold values from -3.912 to -2.526
- forget: float32 [32, 2, 24576], P('tp', None, 'sp'), may hold values from 0 to 2
- wide_input: bfloat16 [2, 32, 64, 16], P(None, 'tp'), may hold values from -1 to 1
- narrow_input: bfloat16 [2, 32, 32, 16], P(None, 'tp'), may hold values from -1 to 1
- wide_output: bfloat16 [2, 32, 16, 64], P(None, 'tp'), may hold values from -0.5 to 0.5
- narrow_output: bfloat16 [2, 32, 16, 32], P(None, 'tp'), may hold values from -0.75 to 0.75
- skip: float32 [1024], P('tp'), may hold values from -4 to 4
- mix_gain: float32 [1024], P('tp'), may hold values from 0.1 to 1.9
- out_weight: bfloat16 [1024, 2048], P('tp'), may hold values from -0.1875 to 0.1875
- mlp_gain: float32 [2048], replicated, may hold values from 0.1 to 1.9
- up_weight: bfloat16 [2048, 8192], P('sp', 'tp'), may hold values from -0.125 to 0.125
- down_weight: bfloat16 [2048, 8192], P('sp', 'tp'), may hold values from -0.0625 to 0.0625
Outputs:
- hidden_out: bfloat16 [24576, 2048], P('sp')
The draws below stay inside these ranges and needn't reach their ends.
Inputs may be any that keep to these rules, and one draw needn't show every extreme that they name: `wide_poles`: entry 0 holds real parts, each at most -1 / 24576; entry 1 holds imaginary parts. `narrow_poles`: entry 0 holds real parts, each at most -1 / 24576; entry 1 holds imaginary parts.
All inputs are finite; a program needn't handle non-finite values.
Results may differ from the reference program's by a relative error of at most 0.02.
Values may be sent and summed in bfloat16 or wider, within the bound.
No kernel may reach another device: no remote copies, remote signals or barrier semaphores. Data moves between devices by JAX's collectives and lax.ppermute only.
A program may use at most 64 MiB of HBM per device.

```python
import math
import jax
import jax.numpy as jnp
from jax import lax

D = 2048
FF = 8192
PAIRS = 32
GROUP = 16
SW = 64
SN = 32
TOK_DEV = 384
TOKEN_POSITIONS = 24576
CHANNELS = 1024
N_TP = 8


def pole_draw(key, state_len):
    random_subkeys = jax.random.split(key, 4)
    slow_share = 0.5
    slow_mask = jax.random.uniform(random_subkeys[0], (PAIRS, 1), jnp.float32) < slow_share
    fast_real = -jax.random.uniform(random_subkeys[1], (PAIRS, state_len), jnp.float32, 0.3, 1.6)
    slow_real = -jax.random.uniform(random_subkeys[2], (PAIRS, state_len), jnp.float32, 0.05, 0.15) / (0.05 * TOKEN_POSITIONS)
    real_part = jnp.where(slow_mask, slow_real, fast_real)
    imag_part = math.pi * jnp.arange(state_len, dtype=jnp.float32)[None, :] + jax.random.uniform(random_subkeys[3], (PAIRS, state_len), jnp.float32, -0.5, 0.5)
    return jnp.stack([real_part, imag_part])


def draw_wide_poles(key, part):
    return pole_draw(jax.random.fold_in(key, 11), SW)


def draw_narrow_poles(key, part):
    return pole_draw(jax.random.fold_in(key, 12), SN)


def draw_forget(key, part):
    random_subkeys = jax.random.split(key, 5)
    devices_along = TOKEN_POSITIONS // TOK_DEV
    parity = jax.random.randint(random_subkeys[0], (), 0, 2)
    parity_sign = jnp.where((jnp.arange(devices_along) + parity) % 2 == 0, 1.0, -1.0)
    block_level = jnp.exp(math.log(2.0) * parity_sign * jax.random.uniform(random_subkeys[1], (devices_along,), jnp.float32, 0.5, 1.0))
    per_position = jnp.repeat(block_level, TOK_DEV, total_repeat_length=TOKEN_POSITIONS)
    rough_low = 0.3
    rough_high = 1.7
    level_scale = 1.0
    roughness = jax.random.uniform(random_subkeys[2], (PAIRS, 2, TOKEN_POSITIONS), jnp.float32, rough_low, rough_high)
    baseline_level = level_scale / TOKEN_POSITIONS * per_position[None, None, :] * roughness
    spike_position = jax.random.randint(random_subkeys[3], (3,), 0, TOKEN_POSITIONS)
    spike_amount = jax.random.uniform(random_subkeys[4], (3,), jnp.float32, 0.22, 0.3)
    spike_signal = jnp.sum((jnp.arange(TOKEN_POSITIONS)[None, :] == spike_position[:, None]).astype(jnp.float32) * spike_amount[:, None], axis=0)
    return baseline_level + spike_signal[None, None, :]


def draw_drive(key, part):
    random_subkeys = jax.random.split(key, 3)
    columns = jnp.arange(CHANNELS, dtype=jnp.float32) / CHANNELS
    column_scale = jnp.exp(math.log(0.5) + math.log(6.0) * columns + jax.random.uniform(random_subkeys[0], (CHANNELS,), jnp.float32, -0.35, 0.35))
    row_scale = jnp.exp(jax.random.uniform(random_subkeys[1], (TOKEN_POSITIONS, 1), jnp.float32, math.log(0.3), math.log(3.2)))
    values = jax.random.normal(random_subkeys[2], (TOKEN_POSITIONS, CHANNELS), jnp.float32)
    return jnp.clip(values * row_scale * column_scale[None, :], -24.0, 24.0).astype(jnp.bfloat16)


def level_of(rng, dims, pieces, smallest, high):
    factor_of, own = 1.0, jax.random.fold_in(rng, 6)
    for dim, shards_of in pieces:
        steps = jnp.exp(jax.random.uniform(jax.random.fold_in(own, dim), (shards_of,), jnp.float32, smallest / len(pieces), high / len(pieces)))
        factor_of = factor_of * jnp.repeat(steps, dims[dim] // shards_of).reshape([-1 if axis == dim else 1 for axis in range(len(dims))])
    return factor_of


def normal_values(own_key, shape, width, limit, cuts=(), kind=jnp.bfloat16):
    drawn = jax.random.normal(own_key, shape, jnp.float32) * width
    if len(cuts) > 0:
        drawn = level_of(own_key, shape, cuts, -0.22, 0.18) * drawn
    return jnp.clip(drawn, min=-limit, max=limit).astype(kind)


def setup_inputs(seed: int = 0) -> dict:
    arg_keys = jax.random.split(jax.random.key(seed), 17)
    return {
        "hidden_in": normal_values(arg_keys[0], (TOKEN_POSITIONS, D), 1.0, 6.0, ((0, 64),)),
        "drive": draw_drive(jax.random.fold_in(arg_keys[16], 71), 0),
        "wide_poles": draw_wide_poles(jax.random.fold_in(arg_keys[16], 71), 0),
        "narrow_poles": draw_narrow_poles(jax.random.fold_in(arg_keys[16], 71), 0),
        "log_step": jnp.clip(-3.912 + 1.3859999 * jax.random.uniform(arg_keys[4], (PAIRS, 2), jnp.float32) ** level_of(arg_keys[4], (PAIRS, 2), ((0, 8),), -0.2, 0.2), -3.912, -2.526),
        "forget": draw_forget(jax.random.fold_in(arg_keys[16], 71), 0),
        "wide_input": normal_values(arg_keys[6], (2, PAIRS, SW, GROUP), (2 * GROUP) ** -0.5, 1.0, ((1, 8),)),
        "narrow_input": normal_values(arg_keys[7], (2, PAIRS, SN, GROUP), (2 * GROUP) ** -0.5, 1.0, ((1, 8),)),
        "wide_output": normal_values(arg_keys[8], (2, PAIRS, GROUP, SW), (2 * SW) ** -0.5, 0.5, ((1, 8),)),
        "narrow_output": normal_values(arg_keys[9], (2, PAIRS, GROUP, SN), (2 * SN) ** -0.5, 0.75, ((1, 8),)),
        "skip": normal_values(arg_keys[10], (CHANNELS,), 1.0, 4.0, ((0, 8),), jnp.float32),
        "mix_gain": jnp.clip(1.0 + 0.18 * jax.random.normal(arg_keys[11], (CHANNELS,), jnp.float32), 0.1, 1.9),
        "out_weight": normal_values(arg_keys[12], (CHANNELS, D), CHANNELS ** -0.5, 0.1875, ((0, 8),)),
        "mlp_gain": jnp.clip(1.0 + 0.18 * jax.random.normal(arg_keys[13], (D,), jnp.float32), 0.1, 1.9),
        "up_weight": normal_values(arg_keys[14], (D, FF), D ** -0.5, 0.125, ((0, 64), (1, 8))),
        "down_weight": normal_values(arg_keys[15], (D, FF), FF ** -0.5, 0.0625, ((0, 64), (1, 8))),
    }


epsilon = 1e-06

def combine(earlier, later):
    return (later[0] * earlier[0] - later[1] * earlier[1], later[0] * earlier[1] + later[1] * earlier[0], later[0] * earlier[2] - later[1] * earlier[3] + later[2], later[0] * earlier[3] + later[1] * earlier[2] + later[3])

def discretize(pole_pair, log_rate):
    step_size = jnp.exp(log_rate)[:, None]
    growth = pole_pair[0] * step_size
    angle = pole_pair[1] * step_size
    rise_real = jnp.expm1(growth) * jnp.cos(angle) - 2.0 * jnp.sin(0.5 * angle) ** 2
    rise_imag = jnp.exp(growth) * jnp.sin(angle)
    denominator = pole_pair[0] ** 2 + pole_pair[1] ** 2
    coef_real = (rise_real * pole_pair[0] + rise_imag * pole_pair[1]) / denominator
    coef_imag = (rise_imag * pole_pair[0] - rise_real * pole_pair[1]) / denominator
    return (growth, angle, coef_real, coef_imag)

def kind_states(signal_rows, decay_rows, terms, in_weight):
    growth, angle, coef_real, coef_imag = terms
    drive_real = jnp.einsum('rpg,psg->rps', signal_rows, in_weight[0].astype(jnp.float32))
    drive_imag = jnp.einsum('rpg,psg->rps', signal_rows, in_weight[1].astype(jnp.float32))
    push_real = coef_real * drive_real - coef_imag * drive_imag
    push_imag = coef_real * drive_imag + coef_imag * drive_real
    spike_magnitude = jnp.exp(growth[None] - decay_rows[:, :, None])
    return lax.associative_scan(combine, (spike_magnitude * jnp.cos(angle)[None], spike_magnitude * jnp.sin(angle)[None], push_real, push_imag), axis=0)

def read_out(state_real, state_imag, out_kind):
    first = jnp.einsum('rps,pgs->rpg', state_real, out_kind[0].astype(jnp.float32), precision=lax.Precision.HIGHEST)
    second = jnp.einsum('rps,pgs->rpg', state_imag, out_kind[1].astype(jnp.float32), precision=lax.Precision.HIGHEST)
    return first - second

def row_norm(rows_in, gain):
    values = rows_in.astype(jnp.float32)
    return (values * lax.rsqrt(lax.optimization_barrier(jnp.mean(values * values, axis=1, keepdims=True)) + epsilon) * gain).astype(jnp.bfloat16)

def reference(hidden_in, drive, wide_poles, narrow_poles, log_step, forget, wide_input, narrow_input, wide_output, narrow_output, skip, mix_gain, out_weight, mlp_gain, up_weight, down_weight):
    block_len = math.gcd(TOKEN_POSITIONS, 512)
    block_count = TOKEN_POSITIONS // block_len
    signal = drive.astype(jnp.float32).reshape(block_count, block_len, PAIRS, 2, GROUP)
    decay_all = jnp.transpose(forget, (2, 0, 1)).reshape(block_count, block_len, PAIRS, 2)
    kinds = ((wide_poles, wide_input, wide_output), (narrow_poles, narrow_input, narrow_output))
    responses = []
    for kind_index in range(2):
        pole_pair, in_weight, out_kind = kinds[kind_index]
        terms = discretize(pole_pair, log_step[:, kind_index])

        def advance(carried, block_inputs):
            cum_real, cum_imag, local_real, local_imag = kind_states(block_inputs[0], block_inputs[1], terms, in_weight)
            state_real = local_real + cum_real * carried[0][None] - cum_imag * carried[1][None]
            state_imag = local_imag + cum_real * carried[1][None] + cum_imag * carried[0][None]
            return ((state_real[-1], state_imag[-1]), read_out(state_real, state_imag, out_kind))
        initial = (jnp.zeros(pole_pair.shape[1:], jnp.float32), jnp.zeros(pole_pair.shape[1:], jnp.float32))
        _, block_outputs = lax.scan(advance, initial, (signal[:, :, :, kind_index], decay_all[:, :, :, kind_index]))
        responses.append(block_outputs.reshape(TOKEN_POSITIONS, PAIRS, GROUP))
    response = jnp.stack(responses, axis=2).reshape(TOKEN_POSITIONS, CHANNELS) + skip[None, :] * drive.astype(jnp.float32)
    active = jax.nn.gelu(response, approximate=False)
    mixed = (active * lax.rsqrt(lax.optimization_barrier(jnp.mean(active * active, axis=1, keepdims=True)) + epsilon) * mix_gain).astype(jnp.bfloat16)
    shard_width = CHANNELS // N_TP
    proj_sum = jnp.zeros((TOKEN_POSITIONS, D), jnp.float32)
    for shard_index in range(N_TP):
        low_edge = shard_index * shard_width
        partial_value = jnp.dot(mixed[:, low_edge:low_edge + shard_width], out_weight[low_edge:low_edge + shard_width], preferred_element_type=jnp.float32)
        proj_sum = proj_sum + lax.optimization_barrier(partial_value.astype(jnp.bfloat16)).astype(jnp.float32)
    carried_rows = (hidden_in.astype(jnp.float32) + proj_sum).astype(jnp.bfloat16)
    normed = row_norm(carried_rows, mlp_gain)
    hidden_width = FF // N_TP
    mixer_sum = jnp.zeros((TOKEN_POSITIONS, D), jnp.float32)
    for shard_index in range(N_TP):
        low_edge = shard_index * hidden_width
        pre_act = jnp.dot(normed, up_weight[:, low_edge:low_edge + hidden_width], preferred_element_type=jnp.float32)
        squared = jnp.square(jax.nn.relu(pre_act)).astype(jnp.bfloat16)
        partial_value = lax.dot_general(squared, down_weight[:, low_edge:low_edge + hidden_width], (((1,), (1,)), ((), ())), preferred_element_type=jnp.float32)
        mixer_sum = mixer_sum + lax.optimization_barrier(partial_value.astype(jnp.bfloat16)).astype(jnp.float32)
    return (carried_rows.astype(jnp.float32) + mixer_sum).astype(jnp.bfloat16)
```

```python
import functools

import jax
import jax.numpy as jnp
from jax import lax
from jax.experimental import pallas as pl
from jax.experimental.pallas import tpu as pltpu
from jax.sharding import PartitionSpec as P

epsilon = 1e-06
bf16, f32 = jnp.bfloat16, jnp.float32
WHOLE = pl.BlockSpec(memory_space=pltpu.VMEM)
SCALARS = pl.BlockSpec(memory_space=pltpu.SMEM)
CHUNKS = 8
LANES = 128
GAIN_ROWS = 16


def copy_for_each(value, axis, groups=None):
    count = len(groups[0]) if groups else lax.axis_size(axis)
    return lax.all_to_all(
        jnp.broadcast_to(value[None], (count, *value.shape)),
        axis,
        0,
        0,
        tiled=True,
        axis_index_groups=groups,
    )


def discretize(pole_pair, log_rate):
    step_size = jnp.exp(log_rate)[:, None]
    growth = pole_pair[0] * step_size
    angle = pole_pair[1] * step_size
    rise_real = jnp.expm1(growth) * jnp.cos(angle) - 2.0 * jnp.sin(0.5 * angle) ** 2
    rise_imag = jnp.exp(growth) * jnp.sin(angle)
    denominator = pole_pair[0] ** 2 + pole_pair[1] ** 2
    coef_real = (rise_real * pole_pair[0] + rise_imag * pole_pair[1]) / denominator
    coef_imag = (rise_imag * pole_pair[0] - rise_real * pole_pair[1]) / denominator
    terms = (growth, jnp.cos(angle), jnp.sin(angle), coef_real, coef_imag)
    return jnp.stack([term.reshape(-1) for term in terms])


def times(a, b):
    return a[0] * b[0] - a[1] * b[1], a[0] * b[1] + a[1] * b[0]


def power_of(phase, exponent):
    result = None
    while exponent:
        if exponent & 1:
            result = phase if result is None else times(result, phase)
        exponent >>= 1
        if exponent:
            phase = times(phase, phase)
    return result


def owners(rows, states, pairs, group, wide):
    row = lax.broadcasted_iota(jnp.int32, (rows, states), 0)
    col = lax.broadcasted_iota(jnp.int32, (rows, states), 1)
    first = pairs * wide
    wide_group = 2 * (col // wide)
    narrow_group = 2 * ((col - first) // ((states - first) // pairs)) + 1
    return row // group == jnp.where(col < first, wide_group, narrow_group)


def spread_blocks(compact, mask, groups):
    states = mask.shape[1]
    tall = jnp.concatenate([compact] * groups, axis=0)
    zero = jnp.zeros((), tall.dtype)
    return jnp.concatenate(
        [jnp.where(mask, tall[:, part * states : (part + 1) * states], zero) for part in range(2)],
        axis=1,
    )


def prepare(dims, drive_ref, forget_ref, terms_ref, in_ref, rows_ref, push_ref, log_ref):
    pairs, group, wide, states = dims
    groups = 2 * pairs
    span = drive_ref.shape[0] // CHUNKS
    for chunk in range(CHUNKS):
        rows_ref[pl.ds(chunk, span, stride=CHUNKS), :] = drive_ref[
            chunk * span : (chunk + 1) * span, :
        ].astype(f32)
    mask = owners(groups * group, states, pairs, group, wide)
    in_block = spread_blocks(in_ref[...].astype(f32), mask, groups).astype(bf16)
    pushed = jnp.dot(rows_ref[...].astype(bf16), in_block, preferred_element_type=f32)
    coef = terms_ref[3:4, :], terms_ref[4:5, :]
    push_real, push_imag = times((pushed[:, :states], pushed[:, states:]), coef)
    push_ref[:, :states] = push_real
    push_ref[:, states:] = push_imag
    spread = owners(groups, states, pairs, 1, wide).astype(f32)
    log_ref[...] = jnp.dot(
        forget_ref[...], spread, precision=lax.Precision.HIGHEST, preferred_element_type=f32
    )


def scan_chunks(states, terms_ref, push_ref, log_ref, start, keep):
    span = push_ref.shape[0] // CHUNKS
    growth = jnp.broadcast_to(terms_ref[0:1, :], (CHUNKS, states))
    cosine = jnp.broadcast_to(terms_ref[1:2, :], (CHUNKS, states))
    sine = jnp.broadcast_to(terms_ref[2:3, :], (CHUNKS, states))

    def one(place, carried):
        real, imag, total = carried
        rows = pl.ds(pl.multiple_of(place * CHUNKS, CHUNKS), CHUNKS)
        forget = log_ref[rows, :]
        decay = jnp.exp(growth - forget)
        turned_real = real * cosine - imag * sine
        turned_imag = real * sine + imag * cosine
        real = decay * turned_real + push_ref[rows, :states]
        imag = decay * turned_imag + push_ref[rows, states:]
        if keep is not None:
            keep(rows, real, imag)
        return real, imag, total + forget

    zero = jnp.zeros((CHUNKS, states), f32)
    return lax.fori_loop(0, span, one, (*start, zero), unroll=8)


def step_factor(terms_ref, forget, length):
    phase = power_of((terms_ref[1:2, :], terms_ref[2:3, :]), length)
    size = jnp.exp(length * terms_ref[0:1, :] - forget)
    return size * phase[0], size * phase[1]


def alternate_lanes(shape):
    return (lax.broadcasted_iota(jnp.int32, shape, len(shape) - 1) // 32) % 2 == 0


def ends_kernel(dims, drive_ref, forget_ref, terms_ref, in_ref, sent_ref, ends_ref, rows_ref, push_ref, log_ref):
    states = dims[3]
    prepare(dims, drive_ref, forget_ref, terms_ref, in_ref, rows_ref, push_ref, log_ref)
    zero = jnp.zeros((CHUNKS, states), f32)
    real, imag, total = scan_chunks(states, terms_ref, push_ref, log_ref, (zero, zero), None)
    ends_ref[0] = real
    ends_ref[1] = imag
    ends_ref[2] = total
    span = push_ref.shape[0] // CHUNKS
    factor = step_factor(terms_ref, total, span)
    state = real[0:1], imag[0:1]
    for chunk in range(1, CHUNKS):
        at = slice(chunk, chunk + 1)
        turned = times((factor[0][at], factor[1][at]), state)
        state = turned[0] + real[at], turned[1] + imag[at]
    whole = jnp.sum(total, axis=0, keepdims=True)
    for part in range(2):
        for tile in range(3):
            sent_ref[3 * part + tile : 3 * part + tile + 1, :] = state[part][
                :, tile * LANES : (tile + 1) * LANES
            ]
    first, second, third = (whole[:, tile * LANES : (tile + 1) * LANES] for tile in range(3))
    sent_ref[6:7, :] = jnp.where(alternate_lanes((1, LANES)), first, second)
    sent_ref[7:8, :] = third


def active_kernel(
    dims,
    here_ref,
    all_ref,
    ends_ref,
    drive_ref,
    forget_ref,
    terms_ref,
    in_ref,
    out_ref,
    skip_ref,
    gain_ref,
    active_ref,
    rows_ref,
    push_ref,
    log_ref,
    state_ref,
):
    pairs, group, wide, states = dims
    prepare(dims, drive_ref, forget_ref, terms_ref, in_ref, rows_ref, push_ref, log_ref)
    length = push_ref.shape[0]
    span = length // CHUNKS

    growth = terms_ref[0:1, :] * length
    phase = power_of((terms_ref[1:2, :], terms_ref[2:3, :]), length)
    even = alternate_lanes((1, LANES))

    def join(tile, at):
        return jnp.concatenate([tile[at + k : at + k + 1, :] for k in range(3)], axis=1)

    def one(device, state):
        tile = all_ref[device]
        packed = tile[6:7, :]
        first = jnp.where(even, packed, pltpu.roll(packed, 32, 1))
        second = jnp.where(even, pltpu.roll(packed, LANES - 32, 1), packed)
        forget = jnp.concatenate([first, second, tile[7:8, :]], axis=1)
        size = jnp.exp(growth - forget)
        turned = times(phase, state)
        return size * turned[0] + join(tile, 0), size * turned[1] + join(tile, 3)

    none = jnp.zeros((1, states), f32)
    state = lax.fori_loop(0, here_ref[0], one, (none, none))

    factor = step_factor(terms_ref, ends_ref[2], span)
    starts = [state]
    for chunk in range(CHUNKS - 1):
        at = slice(chunk, chunk + 1)
        turned = times((factor[0][at], factor[1][at]), state)
        state = turned[0] + ends_ref[0, at], turned[1] + ends_ref[1, at]
        starts.append(state)
    start = tuple(jnp.concatenate([item[part] for item in starts], axis=0) for part in range(2))

    def keep(rows, real, imag):
        state_ref[rows, :states] = real
        state_ref[rows, states:] = imag

    scan_chunks(states, terms_ref, push_ref, log_ref, start, keep)

    mask = owners(2 * pairs * group, states, pairs, group, wide)
    out_block = spread_blocks(out_ref[...].astype(f32), mask, 2 * pairs).astype(bf16)
    value = state_ref[...]
    high = value.astype(bf16)
    low = (value - high.astype(f32)).astype(bf16)
    over = (((1,), (1,)), ((), ()))
    response = lax.dot_general(high, out_block, over, preferred_element_type=f32)
    response = response + lax.dot_general(low, out_block, over, preferred_element_type=f32)
    response = response + skip_ref[...] * rows_ref[...]
    rows_ref[...] = 0.5 * response * (1.0 + lax.erf(response * 0.7071067811865476))
    for chunk in range(CHUNKS):
        active_ref[chunk * span : (chunk + 1) * span, :] = rows_ref[
            pl.ds(chunk, span, stride=CHUNKS), :
        ].astype(bf16)
    gain, parts = gain_ref[...], []
    for _ in range(3):
        parts.append(gain.astype(bf16))
        gain = gain - parts[-1].astype(f32)
    parts.append(jnp.zeros((GAIN_ROWS - 3, gain.shape[1]), bf16))
    active_ref[length:, :] = jnp.concatenate(parts, axis=0)


def normed_kernel(here_ref, act_ref, gain_ref, same_ref, other_ref, hidden_ref, mlp_ref, normed_ref, own_ref):
    chip, core = here_ref[0] // 2, here_ref[0] % 2
    chips = same_ref.shape[0]
    active = act_ref[...].astype(f32)
    power = jnp.sum(jnp.sum(active * active, axis=0), axis=1, keepdims=True)
    channels = act_ref.shape[0] * act_ref.shape[2]
    scale = lax.rsqrt(power / channels + epsilon)

    def mixed(block):
        gain = jnp.sum(gain_ref[block].astype(f32), axis=0, keepdims=True)
        return (act_ref[block].astype(f32) * scale * gain).astype(bf16)

    total = jnp.zeros(hidden_ref.shape, f32)
    for back in range(chips):
        base = 2 * lax.rem(chip + chips - back, chips)
        total += jnp.dot(mixed(base + core), same_ref[back], preferred_element_type=f32)
        total += jnp.dot(mixed(base + 1 - core), other_ref[back], preferred_element_type=f32)
    carried = (hidden_ref[...].astype(f32) + total).astype(bf16)
    values = carried.astype(f32)
    normed_ref[...] = (
        values * lax.rsqrt(jnp.mean(values * values, axis=1, keepdims=True) + epsilon) * mlp_ref[...]
    ).astype(bf16)

    @pl.when(pl.program_id(0) == here_ref[0])
    def _():
        own_ref[...] = carried


def mixer_kernel(here_ref, normed_ref, weight_ref, own_ref, other_ref, up_ref, down_ref, up_sem, down_sem):
    blocks, parts = up_sem.shape[0], up_ref.shape[0] // up_sem.shape[0]
    width = up_ref.shape[1]

    def copies(block):
        at = pl.ds(block * parts, parts)
        return (
            pltpu.make_async_copy(weight_ref.at[at, pl.ds(0, width), :], up_ref.at[at], up_sem.at[block]),
            pltpu.make_async_copy(
                weight_ref.at[at, pl.ds(width, width), :], down_ref.at[at], down_sem.at[block]
            ),
        )

    for which in range(2):
        for block in range(blocks):
            copies(block)[which].start()
    rows, hidden = normed_ref.shape[0], up_ref.shape[2]
    depth = parts * width
    total = jnp.zeros((rows, hidden), f32)
    for block in range(blocks):
        copies(block)[0].wait()
        piece = up_ref[block * parts : (block + 1) * parts].reshape(depth, hidden)
        total += jnp.dot(
            normed_ref[:, block * depth : (block + 1) * depth], piece, preferred_element_type=f32
        )
    squared = jnp.square(jnp.maximum(total, 0.0)).astype(bf16)
    core = here_ref[0] % 2
    share = own_ref.shape[1]
    for block in range(blocks):
        copies(block)[1].wait()
        piece = down_ref[block * parts : (block + 1) * parts].reshape(depth, hidden)
        value = lax.dot_general(
            squared, piece, (((1,), (1,)), ((), ())), preferred_element_type=f32
        ).astype(bf16)
        value = value.reshape(own_ref.shape[0], 2, share, depth)
        at = slice(block * depth, (block + 1) * depth)
        own_ref[:, :, at] = jnp.where(core == 0, value[:, 0], value[:, 1])
        other_ref[:, :, at] = jnp.where(core == 0, value[:, 1], value[:, 0])


def local(
    hidden_in,
    drive,
    wide_poles,
    narrow_poles,
    log_step,
    forget,
    wide_input,
    narrow_input,
    wide_output,
    narrow_output,
    skip,
    mix_gain,
    out_weight,
    mlp_gain,
    up_weight,
    down_weight,
):
    rows, model = hidden_in.shape
    count = lax.axis_size("tp")
    chips, share = count // 2, rows // count
    pairs, wide = wide_poles.shape[1:]
    group = wide_input.shape[3]
    states = pairs * (wide + narrow_poles.shape[2])
    dims = (pairs, group, wide, states)
    here = lax.axis_index("tp").reshape(1)
    same_core = [[2 * chip + core for chip in range(chips)] for core in range(2)]

    weights = lax.all_gather(jnp.concatenate([up_weight, down_weight], axis=0), "sp", axis=0)

    def from_chip(value, back):
        return lax.ppermute(value, "tp", [(i, (i + 2 * back) % count) for i in range(count)])

    def swap(value):
        return lax.ppermute(value, "tp", [(i, i ^ 1) for i in range(count)])

    out_same = jnp.stack([out_weight] + [from_chip(out_weight, back) for back in range(1, chips)])
    out_other = swap(out_same)

    terms = jnp.concatenate(
        [discretize(wide_poles, log_step[:, 0]), discretize(narrow_poles, log_step[:, 1])], axis=1
    )
    forget_rows = jnp.transpose(
        forget.reshape(2 * pairs, CHUNKS, rows // CHUNKS), (2, 1, 0)
    ).reshape(rows, 2 * pairs)

    def compact(first, second, order):
        first, second = (
            jnp.transpose(item, order).reshape(group, 2, -1) for item in (first, second)
        )
        return jnp.concatenate([first, second], axis=2).reshape(group, 2 * states)

    in_compact = compact(wide_input, narrow_input, (3, 0, 1, 2))
    out_compact = compact(
        wide_output * jnp.array([1, -1], bf16)[:, None, None, None],
        narrow_output * jnp.array([1, -1], bf16)[:, None, None, None],
        (2, 0, 1, 3),
    )
    channels = drive.shape[1]
    scratch = [
        pltpu.VMEM((rows, channels), f32),
        pltpu.VMEM((rows, 2 * states), f32),
        pltpu.VMEM((rows, states), f32),
    ]
    sent, ends = pl.pallas_call(
        functools.partial(ends_kernel, dims),
        out_shape=[
            jax.ShapeDtypeStruct((8, LANES), f32),
            jax.ShapeDtypeStruct((3, CHUNKS, states), f32),
        ],
        in_specs=[WHOLE] * 4,
        out_specs=[WHOLE] * 2,
        scratch_shapes=scratch,
        name="ends",
    )(drive, forget_rows, terms, in_compact)
    everyone = copy_for_each(sent[None], "sp").reshape(-1, *sent.shape)
    active = pl.pallas_call(
        functools.partial(active_kernel, dims),
        out_shape=jax.ShapeDtypeStruct((rows + GAIN_ROWS, channels), bf16),
        in_specs=[SCALARS] + [WHOLE] * 9,
        out_specs=WHOLE,
        scratch_shapes=scratch + [pltpu.VMEM((rows, 2 * states), f32)],
        name="active",
    )(
        lax.axis_index("sp").reshape(1),
        everyone,
        ends,
        drive,
        forget_rows,
        terms,
        in_compact,
        out_compact,
        skip[None],
        mix_gain[None],
    )
    gathered = lax.all_gather(active, "tp", axis=0)
    normed, own_rows = pl.pallas_call(
        normed_kernel,
        grid=(count,),
        out_shape=[
            jax.ShapeDtypeStruct((rows, model), bf16),
            jax.ShapeDtypeStruct((share, model), bf16),
        ],
        in_specs=[
            SCALARS,
            pl.BlockSpec((count, share, channels), lambda i: (0, i, 0)),
            pl.BlockSpec((count, GAIN_ROWS, channels), lambda i: (0, rows // GAIN_ROWS, 0)),
            pl.BlockSpec(out_same.shape, lambda i: (0, 0, 0)),
            pl.BlockSpec(out_same.shape, lambda i: (0, 0, 0)),
            pl.BlockSpec((share, model), lambda i: (i, 0)),
            pl.BlockSpec((1, model), lambda i: (0, 0)),
        ],
        out_specs=[
            pl.BlockSpec((share, model), lambda i: (i, 0)),
            pl.BlockSpec((share, model), lambda i: (0, 0)),
        ],
        name="normed",
    )(here, gathered, gathered, out_same, out_other, hidden_in, mlp_gain[None])
    devices, width, hidden = weights.shape[0], up_weight.shape[0], up_weight.shape[1]
    own_part, other_part = pl.pallas_call(
        mixer_kernel,
        out_shape=[jax.ShapeDtypeStruct((chips, share, model), bf16)] * 2,
        in_specs=[SCALARS, WHOLE, pl.BlockSpec(memory_space=pl.ANY)],
        out_specs=[WHOLE] * 2,
        scratch_shapes=[
            pltpu.VMEM((devices, width, hidden), bf16),
            pltpu.VMEM((devices, width, hidden), bf16),
            pltpu.SemaphoreType.DMA((8,)),
            pltpu.SemaphoreType.DMA((8,)),
        ],
        name="mixer",
    )(here, normed, weights)
    chip_part = (own_part.astype(f32) + swap(other_part).astype(f32)).astype(bf16)
    pieces = lax.all_to_all(chip_part, "tp", 0, 0, tiled=True, axis_index_groups=same_core)
    total = jnp.sum(pieces.astype(f32), axis=0)
    finished = (own_rows.astype(f32) + total).astype(bf16)
    mine = copy_for_each(finished[None], "tp", same_core)
    theirs = swap(mine)
    first = here[0] % 2 == 0
    return jnp.stack(
        [jnp.where(first, mine, theirs), jnp.where(first, theirs, mine)], axis=1
    ).reshape(rows, model)


def solution(mesh):
    return jax.shard_map(
        local,
        mesh=mesh,
        in_specs=(
            P("sp", None),
            P("sp", "tp"),
            P(None, "tp", None),
            P(None, "tp", None),
            P("tp", None),
            P("tp", None, "sp"),
            P(None, "tp", None, None),
            P(None, "tp", None, None),
            P(None, "tp", None, None),
            P(None, "tp", None, None),
            P("tp"),
            P("tp"),
            P("tp", None),
            P(),
            P("sp", "tp"),
            P("sp", "tp"),
        ),
        out_specs=P("sp", None),
        check_vma=False,
    )
```
